512 devices in a mesh: fs: 128 (over z, x, core), tp: 4 (over y).
Axes of the slice: x: 4, y: 4, z: 16, core: 2. Of those that a mesh axis runs over, the one named last changes fastest.
Arguments:
- normed_input: bfloat16 [131072, 2048], P('fs'), may hold values from -64 to 64
- query_cotangent: bfloat16 [131072, 1024], P('fs', 'tp'), may hold values from -6 to 6
- key_cotangent: bfloat16 [131072, 512], P('fs', 'tp'), may hold values from -6 to 6
- query_weight: float32 [2048, 1024], P('fs', 'tp'), may hold values from -6 to 6
- key_weight: float32 [2048, 512], P('fs', 'tp'), may hold values from -6 to 6
- query_basis: bfloat16 [1024, 128], P('tp'), may hold values from -1 to 1
- key_basis: bfloat16 [512, 128], P('tp'), may hold values from -1 to 1
- moment_mean: float32 [2, 2048, 128], P(None, 'fs'), may hold values from -3 to 3
- moment_square: float32 [2, 2048, 128], P(None, 'fs'), may hold values from 0.25 to 4
Outputs:
- query_step: float32 [2048, 1024], P('fs', 'tp')
- key_step: float32 [2048, 512], P('fs', 'tp')
- query_updated: float32 [2048, 1024], P('fs', 'tp')
- key_updated: float32 [2048, 512], P('fs', 'tp')
- query_copy: bfloat16 [2048, 1024], P('fs', 'tp')
- key_copy: bfloat16 [2048, 512], P('fs', 'tp')
- mean_updated: float32 [2, 2048, 128], P(None, 'fs')
- square_updated: float32 [2, 2048, 128], P(None, 'fs')
The draws below stay inside these ranges and needn't reach their ends.
All inputs are finite; a program needn't handle non-finite values.
Results may differ from the reference program's by a relative error of at most 0.0011.
Values sent between devices are 32-bit elements; how exact they have to be, the bound alone decides.
No kernel may reach another device: no remote copies, remote signals or barrier semaphores. Data moves between devices by JAX's collectives and lax.ppermute only.
A program may use at most 64 MiB of HBM per device.

```python
import math
import jax
import jax.numpy as jnp
from jax import lax

D = 2048
QUERY_WIDTH = 1024
KEY_WIDTH = 512
RANK = 128
TOKENS = 131072
N_FS = 128


def draw_normed_input(key, part):
    first_key, second_key = jax.random.split(jax.random.fold_in(key, 17), 2)
    position = jnp.arange(D, dtype=jnp.float32) / D
    roughness = jnp.exp(jax.random.uniform(second_key, (D,), jnp.float32, -0.7, 0.7))
    entries = jax.random.normal(first_key, (TOKENS, D), jnp.float32)
    values = entries * 10.0 ** position * roughness
    return jnp.clip(values, -64.0, 64.0).astype(jnp.bfloat16)


def factor_draw(key, row_count, offset_seed):
    first_key, second_key = jax.random.split(jax.random.fold_in(key, offset_seed))
    entries = jax.random.normal(first_key, (row_count, RANK), jnp.float32)
    spread = jnp.exp(jax.random.uniform(second_key, (RANK,), jnp.float32, -1.15, 1.15))
    values = entries * spread / jnp.sqrt(jnp.float32(row_count))
    return jnp.clip(values, -1.0, 1.0).astype(jnp.bfloat16)


def draw_query_basis(key, part):
    return factor_draw(key, QUERY_WIDTH, 31)


def draw_key_basis(key, part):
    return factor_draw(key, KEY_WIDTH, 43)


def block_scale(rng, shape, pieces, least, top_value):
    def one(dim, shards_of):
        heights = jax.random.uniform(jax.random.fold_in(jax.random.fold_in(rng, 6), dim), (shards_of,), jnp.float32, least / len(pieces), top_value / len(pieces))
        return jnp.repeat(jnp.exp(heights), shape[dim] // shards_of).reshape((-1,) + (1,) * (len(shape) - dim - 1))

    loudness = one(*pieces[0])
    for cut in pieces[1:]:
        loudness = loudness * one(*cut)
    return loudness


def centred(rng, dims, scale, most, cuts=(), held_as=jnp.bfloat16):
    values = jax.random.normal(rng, dims, jnp.float32) * scale
    if len(cuts) > 0:
        values = block_scale(rng, dims, cuts, -0.22, 0.18) * values
    return jnp.clip(values, min=-most, max=most).astype(held_as)


def setup_inputs(seed: int = 0) -> dict:
    key_list = jax.random.split(jax.random.key(seed), 10)
    return {
        "normed_input": draw_normed_input(jax.random.fold_in(key_list[9], 71), 0),
        "query_cotangent": centred(key_list[1], (TOKENS, QUERY_WIDTH), 1.0, 6.0, ((0, 128), (1, 4))),
        "key_cotangent": centred(key_list[2], (TOKENS, KEY_WIDTH), 1.0, 6.0, ((0, 128), (1, 4))),
        "query_weight": centred(key_list[3], (D, QUERY_WIDTH), 1.0, 6.0, ((0, 128), (1, 4)), jnp.float32),
        "key_weight": centred(key_list[4], (D, KEY_WIDTH), 1.0, 6.0, ((0, 128), (1, 4)), jnp.float32),
        "query_basis": draw_query_basis(jax.random.fold_in(key_list[9], 71), 0),
        "key_basis": draw_key_basis(jax.random.fold_in(key_list[9], 71), 0),
        "moment_mean": centred(key_list[7], (2, D, RANK), 0.5, 3.0, ((1, 128),), jnp.float32),
        "moment_square": jnp.clip(jnp.exp(math.log(4.0) - 2.7725887 * jax.random.uniform(key_list[8], (2, D, RANK), jnp.float32) ** block_scale(key_list[8], (2, D, RANK), ((1, 128),), -0.2, 0.2)), 0.25, 4.0),
    }


BETA_MEAN = 0.75
BETA_SQUARE = 0.8
STEP_RATE = 0.25
EPSILON = 1e-06

def gradient_sum(inputs, cotangent):
    columns = cotangent.shape[1]
    input_blocks = inputs.reshape(N_FS, inputs.shape[0] // N_FS, inputs.shape[1])
    cotangent_blocks = cotangent.reshape(N_FS, cotangent.shape[0] // N_FS, columns)

    def accumulate(running_sum, operands):
        input_rows, cotangent_rows = operands
        product = lax.dot_general(input_rows.astype(jnp.float32), cotangent_rows.astype(jnp.float32), (((0,), (0,)), ((), ())), precision=lax.Precision.HIGHEST, preferred_element_type=jnp.float32)
        return (running_sum + product, None)
    initial = jnp.zeros((inputs.shape[1], columns), jnp.float32)
    running_sum, unused = lax.scan(accumulate, initial, (input_blocks, cotangent_blocks))
    return running_sum

def reference(normed_input, query_cotangent, key_cotangent, query_weight, key_weight, query_basis, key_basis, moment_mean, moment_square):
    query_float = query_basis.astype(jnp.float32)
    key_float = key_basis.astype(jnp.float32)
    query_gradient = gradient_sum(normed_input, query_cotangent)
    key_gradient = gradient_sum(normed_input, key_cotangent)
    query_projected = jnp.dot(query_gradient, query_float, precision=lax.Precision.HIGHEST)
    key_projected = jnp.dot(key_gradient, key_float, precision=lax.Precision.HIGHEST)
    projected = jnp.stack([query_projected, key_projected])
    mean_square = jnp.sum(projected * projected) / (2.0 * projected.shape[1] * projected.shape[2])
    normalized = projected * lax.rsqrt(mean_square + EPSILON)
    mean_updated = BETA_MEAN * moment_mean + (1.0 - BETA_MEAN) * normalized
    square_updated = BETA_SQUARE * moment_square + (1.0 - BETA_SQUARE) * normalized * normalized
    direction = mean_updated / jnp.sqrt(square_updated)
    query_step = jnp.dot(direction[0], query_float.T, precision=lax.Precision.HIGHEST)
    key_step = jnp.dot(direction[1], key_float.T, precision=lax.Precision.HIGHEST)
    query_updated = query_weight - STEP_RATE * query_step
    key_updated = key_weight - STEP_RATE * key_step
    return (query_step, key_step, query_updated, key_updated, query_updated.astype(jnp.bfloat16), key_updated.astype(jnp.bfloat16), mean_updated, square_updated)
```

```python
import jax
import jax.numpy as jnp
from jax import lax
from jax.experimental import pallas as pl
from jax.experimental.pallas import tpu as pltpu
from jax.sharding import Mesh
from jax.sharding import PartitionSpec as P

FS = ("fs_0", "fs_1", "fs_2")

BETA_MEAN = 0.75
BETA_SQUARE = 0.8
STEP_RATE = 0.25
EPSILON = 1e-06
BLOCK = 256

HIGHEST = lax.Precision.HIGHEST
OUTER = (((1,), (1,)), ((), ()))
TOKENS_OUT = (((0,), (0,)), ((), ()))


def dot(a, b, dims, precision=None):
    return lax.dot_general(a, b, dims, precision=precision, preferred_element_type=jnp.float32)


def halves(value):
    high = value.astype(jnp.bfloat16)
    low = (value - high.astype(jnp.float32)).astype(jnp.bfloat16)
    return high, low


def store_block(x_ref, factor, out_ref):
    both = dot(x_ref[...], factor, TOKENS_OUT)
    rank = both.shape[1] // 2
    part = both[:, :rank] + both[:, rank:]
    zs, rows = out_ref.shape[1], out_ref.shape[0] * out_ref.shape[2]
    for z in range(zs):
        piece = part[z * rows : (z + 1) * rows]
        out_ref[:, z, :, :] = piece.reshape(out_ref.shape[0], out_ref.shape[2], rank)


def other_kernel(core, cq_ref, ck_ref, bq_ref, bk_ref, x_ref, out_ref, own_ref, other_ref):
    @pl.when(pl.program_id(0) == 0)
    def _():
        rank = bq_ref.shape[1]
        query = dot(cq_ref[...], bq_ref[...], (((1,), (0,)), ((), ())))
        key = dot(ck_ref[...], bk_ref[...], (((1,), (0,)), ((), ())))
        is_query = core[0] == 0
        own_high, own_low = halves(jnp.where(is_query, query, key))
        own_ref[:, :rank] = own_high
        own_ref[:, rank:] = own_low
        other_high, other_low = halves(jnp.where(is_query, key, query))
        other_ref[:, :rank] = other_high
        other_ref[:, rank:] = other_low

    store_block(x_ref, other_ref[...], out_ref)


def own_kernel(own_ref, x_ref, out_ref):
    store_block(x_ref, own_ref[...], out_ref)


def last_kernel(
    core, squares_ref, tiles_ref, mean_ref, square_ref, bq_ref, bk_ref, wq_ref, wk_ref,
    qs_ref, ks_ref, qu_ref, ku_ref, qc_ref, kc_ref, mean_out, square_out, *, entry_count,
):
    total = jnp.sum(squares_ref[...].reshape(-1, squares_ref.shape[-1]), axis=0, keepdims=True)
    total = jnp.sum(total, axis=1, keepdims=True)
    scale = lax.rsqrt(total / entry_count + EPSILON)
    groups = tiles_ref.shape[0] // 2
    mine = groups // 2
    rows, rank = mean_ref.shape[1], mean_ref.shape[2]
    for which, basis, weight, step_ref, up_ref, copy_ref in (
        (0, bq_ref, wq_ref, qs_ref, qu_ref, qc_ref),
        (1, bk_ref, wk_ref, ks_ref, ku_ref, kc_ref),
    ):
        tile = tiles_ref[pl.ds(which * groups + core[0] * mine, mine)].reshape(rows, rank)
        normalized = tile * scale
        mean = BETA_MEAN * mean_ref[which] + (1.0 - BETA_MEAN) * normalized
        square = BETA_SQUARE * square_ref[which] + (1.0 - BETA_SQUARE) * normalized * normalized
        mean_out[which] = mean
        square_out[which] = square
        direction = mean / jnp.sqrt(square)
        step = dot(direction, basis[...].astype(jnp.float32), OUTER, HIGHEST)
        step_ref[...] = step
        updated = weight[...] - STEP_RATE * step
        up_ref[...] = updated
        copy_ref[...] = updated.astype(jnp.bfloat16)


def whole(shape):
    return pl.BlockSpec(shape, lambda *i: (0,) * len(shape))


def local(
    normed_input,
    query_cotangent,
    key_cotangent,
    query_weight,
    key_weight,
    query_basis,
    key_basis,
    moment_mean,
    moment_square,
):
    far, near, cores, heads = (lax.axis_size(a) for a in ("fs_0", "fs_1", "fs_2", "tp"))
    core = lax.axis_index("fs_2").astype(jnp.int32).reshape(1)
    tokens, width = normed_input.shape
    rank = query_basis.shape[1]
    tile = width // (far * near * heads)
    planes = BLOCK // (width // far)
    sums = jax.ShapeDtypeStruct((near * heads, far, tile, rank), jnp.float32)
    x_spec = pl.BlockSpec((tokens, BLOCK), lambda i, *_: (0, i))
    out_spec = pl.BlockSpec((near * heads, planes, tile, rank), lambda i, *_: (0, i, 0, 0))
    cost = pl.CostEstimate(
        flops=4 * tokens * width * rank, bytes_accessed=2 * tokens * width + 4 * width * rank, transcendentals=0
    )
    factor = jax.ShapeDtypeStruct((tokens, 2 * rank), jnp.bfloat16)
    other, own_factor = pl.pallas_call(
        other_kernel,
        grid_spec=pltpu.PrefetchScalarGridSpec(
            num_scalar_prefetch=1,
            grid=(width // BLOCK,),
            in_specs=[
                whole(query_cotangent.shape),
                whole(key_cotangent.shape),
                whole(query_basis.shape),
                whole(key_basis.shape),
                x_spec,
            ],
            out_specs=[out_spec, whole(factor.shape)],
            scratch_shapes=[pltpu.VMEM(factor.shape, factor.dtype)],
        ),
        out_shape=[sums, factor],
        cost_estimate=cost,
        compiler_params=pltpu.CompilerParams(vmem_limit_bytes=16 << 20),
    )(core, query_cotangent, key_cotangent, query_basis, key_basis, normed_input)
    received = lax.ppermute(other, "fs_2", [(0, 1), (1, 0)])
    own = pl.pallas_call(
        own_kernel,
        grid=(width // BLOCK,),
        in_specs=[whole(factor.shape), x_spec],
        out_specs=out_spec,
        out_shape=sums,
        cost_estimate=cost,
        compiler_params=pltpu.CompilerParams(vmem_limit_bytes=16 << 20),
    )(own_factor, normed_input)
    chip = own + received
    plane = jnp.sum(lax.all_to_all(chip, ("fs_1", "tp"), 0, 0, tiled=True), axis=0)
    mine = jnp.sum(lax.all_to_all(plane, "fs_0", 0, 0, tiled=True), axis=0)
    sent = jnp.broadcast_to(mine[None], (cores * heads, tile, rank))
    tiles = lax.all_to_all(sent, ("fs_2", "tp"), 0, 0, tiled=True)
    squares = jnp.sum(tiles * tiles, axis=(0, 1))
    squares = jnp.broadcast_to(squares.reshape(1, 1, rank), (far * near, 1, rank))
    squares = lax.all_to_all(squares, ("fs_0", "fs_1"), 0, 0, tiled=True)
    entry_count = 2.0 * width * rank
    like = lambda a, dtype=None: jax.ShapeDtypeStruct(a.shape, dtype or a.dtype)
    smem = pl.BlockSpec(memory_space=pltpu.SMEM)
    vmem = pl.BlockSpec(memory_space=pltpu.VMEM)
    return pl.pallas_call(
        lambda *refs: last_kernel(*refs, entry_count=entry_count),
        in_specs=[smem] + [vmem] * 8,
        out_specs=[vmem] * 8,
        out_shape=[
            like(query_weight),
            like(key_weight),
            like(query_weight),
            like(key_weight),
            like(query_weight, jnp.bfloat16),
            like(key_weight, jnp.bfloat16),
            like(moment_mean),
            like(moment_square),
        ],
        compiler_params=pltpu.CompilerParams(vmem_limit_bytes=8 << 20),
    )(
        core,
        squares.reshape(far * near, rank),
        tiles,
        moment_mean,
        moment_square,
        query_basis,
        key_basis,
        query_weight,
        key_weight,
    )


def solution(mesh):
    split = Mesh(mesh.devices.reshape(16, 4, 2, mesh.shape["tp"]), ("fs_0", "fs_1", "fs_2", "tp"))
    in_specs = (
        P(FS, None),
        P(FS, "tp"),
        P(FS, "tp"),
        P(FS, "tp"),
        P(FS, "tp"),
        P("tp", None),
        P("tp", None),
        P(None, FS, None),
        P(None, FS, None),
    )
    out_specs = (
        P(FS, "tp"),
        P(FS, "tp"),
        P(FS, "tp"),
        P(FS, "tp"),
        P(FS, "tp"),
        P(FS, "tp"),
        P(None, FS, None),
        P(None, FS, None),
    )
    return jax.shard_map(local, mesh=split, in_specs=in_specs, out_specs=out_specs, check_vma=False)
```

```python
import jax
import jax.numpy as jnp
from jax import lax
from jax.experimental import pallas as pl
from jax.experimental.pallas import tpu as pltpu
from jax.sharding import Mesh
from jax.sharding import PartitionSpec as P

FS = ("fs_0", "fs_1", "fs_2")

BETA_MEAN = 0.75
BETA_SQUARE = 0.8
STEP_RATE = 0.25
EPSILON = 1e-06
BLOCK = 512

HIGHEST = lax.Precision.HIGHEST
OUTER = (((1,), (1,)), ((), ()))
TOKENS_OUT = (((0,), (0,)), ((), ()))


def dot(a, b, dims, precision=None):
    return lax.dot_general(a, b, dims, precision=precision, preferred_element_type=jnp.float32)


def halves(value):
    high = value.astype(jnp.bfloat16)
    low = (value - high.astype(jnp.float32)).astype(jnp.bfloat16)
    return high, low


def store_block(x, factor, out_ref, first):
    both = dot(x, factor, TOKENS_OUT)
    rank = both.shape[1] // 2
    part = both[:, :rank] + both[:, rank:]
    groups, _, tile, _ = out_ref.shape
    for start in range(0, part.shape[0], groups * tile):
        piece = part[start : start + groups * tile]
        out_ref[:, (first + start) // (groups * tile), :, :] = piece.reshape(groups, tile, rank)


def other_kernel(
    core, x_hbm, cq_hbm, ck_hbm, bq_hbm, bk_hbm, out_ref, own_ref, x_ref,
    cq_ref, ck_ref, bq_ref, bk_ref, other_ref, sems, x_sems,
):
    copies = [
        pltpu.make_async_copy(source, target, sems.at[i])
        for i, (source, target) in enumerate(
            ((cq_hbm, cq_ref), (bq_hbm, bq_ref), (ck_hbm, ck_ref), (bk_hbm, bk_ref))
        )
    ]
    width = x_ref.shape[1]
    columns = [slice(i, i + BLOCK) for i in range(0, width, BLOCK)]
    blocks = [
        pltpu.make_async_copy(x_hbm.at[:, c], x_ref.at[:, c], x_sems.at[i]) for i, c in enumerate(columns)
    ]
    for copy in copies + blocks:
        copy.start()
    for copy in copies:
        copy.wait()
    rank = bq_ref.shape[1]
    query = dot(cq_ref[...], bq_ref[...], (((1,), (0,)), ((), ())))
    key = dot(ck_ref[...], bk_ref[...], (((1,), (0,)), ((), ())))
    is_query = core[0] == 0
    own_high, own_low = halves(jnp.where(is_query, query, key))
    own_ref[:, :rank] = own_high
    own_ref[:, rank:] = own_low
    other_high, other_low = halves(jnp.where(is_query, key, query))
    other_ref[:, :rank] = other_high
    other_ref[:, rank:] = other_low
    for c, copy in zip(columns, blocks):
        copy.wait()
        store_block(x_ref[:, c], other_ref[...], out_ref, c.start)


def own_kernel(own_ref, x_ref, out_ref):
    for start in range(0, x_ref.shape[1], BLOCK):
        store_block(x_ref[:, start : start + BLOCK], own_ref[...], out_ref, start)


def last_kernel(
    core, squares_ref, tiles_ref, mean_ref, square_ref, bq_ref, bk_ref, wq_ref, wk_ref,
    qs_ref, ks_ref, qu_ref, ku_ref, qc_ref, kc_ref, mean_out, square_out, *, entry_count,
):
    total = jnp.sum(squares_ref[...].reshape(-1, squares_ref.shape[-1]), axis=0, keepdims=True)
    total = jnp.sum(total, axis=1, keepdims=True)
    scale = lax.rsqrt(total / entry_count + EPSILON)
    groups = tiles_ref.shape[0] // 2
    mine = groups // 2
    rows, rank = mean_ref.shape[1], mean_ref.shape[2]
    for which, basis, weight, step_ref, up_ref, copy_ref in (
        (0, bq_ref, wq_ref, qs_ref, qu_ref, qc_ref),
        (1, bk_ref, wk_ref, ks_ref, ku_ref, kc_ref),
    ):
        tile = tiles_ref[pl.ds(which * groups + core[0] * mine, mine)].reshape(rows, rank)
        normalized = tile * scale
        mean = BETA_MEAN * mean_ref[which] + (1.0 - BETA_MEAN) * normalized
        square = BETA_SQUARE * square_ref[which] + (1.0 - BETA_SQUARE) * normalized * normalized
        mean_out[which] = mean
        square_out[which] = square
        direction = mean / jnp.sqrt(square)
        step = dot(direction, basis[...].astype(jnp.float32), OUTER, HIGHEST)
        step_ref[...] = step
        updated = weight[...] - STEP_RATE * step
        up_ref[...] = updated
        copy_ref[...] = updated.astype(jnp.bfloat16)


def whole(shape):
    return pl.BlockSpec(shape, lambda *i: (0,) * len(shape))


def local(
    normed_input,
    query_cotangent,
    key_cotangent,
    query_weight,
    key_weight,
    query_basis,
    key_basis,
    moment_mean,
    moment_square,
):
    far, near, cores, heads = (lax.axis_size(a) for a in ("fs_0", "fs_1", "fs_2", "tp"))
    core = lax.axis_index("fs_2").astype(jnp.int32).reshape(1)
    tokens, width = normed_input.shape
    rank = query_basis.shape[1]
    tile = width // (far * near * heads)
    sums = pltpu.VMEM((near * heads, far, tile, rank), jnp.float32)
    cost = pl.CostEstimate(
        flops=4 * tokens * width * rank, bytes_accessed=2 * tokens * width + 4 * width * rank, transcendentals=0
    )
    params = pltpu.CompilerParams(vmem_limit_bytes=16 << 20)
    factor = pltpu.VMEM((tokens, 2 * rank), jnp.bfloat16)
    sources = (normed_input, query_cotangent, key_cotangent, query_basis, key_basis)
    hbm = pl.BlockSpec(memory_space=pltpu.HBM)
    vmem = pl.BlockSpec(memory_space=pltpu.VMEM)
    smem = pl.BlockSpec(memory_space=pltpu.SMEM)
    other, own_factor, held = pl.pallas_call(
        other_kernel,
        in_specs=[smem] + [hbm] * len(sources),
        out_specs=[vmem] * 3,
        out_shape=[sums, factor, pltpu.VMEM(normed_input.shape, normed_input.dtype)],
        scratch_shapes=[pltpu.VMEM(a.shape, a.dtype) for a in sources[1:3] + sources[3:]]
        + [factor, pltpu.SemaphoreType.DMA((4,)), pltpu.SemaphoreType.DMA((width // BLOCK,))],
        cost_estimate=cost,
        compiler_params=params,
    )(core, *(pltpu.with_memory_space_constraint(a, pltpu.HBM) for a in sources))
    received = lax.ppermute(other, "fs_2", [(0, 1), (1, 0)])
    own = pl.pallas_call(
        own_kernel,
        in_specs=[vmem] * 2,
        out_specs=vmem,
        out_shape=sums,
        cost_estimate=cost,
        compiler_params=params,
    )(own_factor, held)
    chip = own + received
    plane = jnp.sum(lax.all_to_all(chip, ("fs_1", "tp"), 0, 0, tiled=True), axis=0)
    mine = jnp.sum(lax.all_to_all(plane, "fs_0", 0, 0, tiled=True), axis=0)
    sent = jnp.broadcast_to(mine[None], (cores * heads, tile, rank))
    tiles = lax.all_to_all(sent, ("fs_2", "tp"), 0, 0, tiled=True)
    squares = jnp.sum(tiles * tiles, axis=(0, 1))
    squares = jnp.broadcast_to(squares.reshape(1, 1, rank), (far * near, 1, rank))
    squares = lax.all_to_all(squares, ("fs_0", "fs_1"), 0, 0, tiled=True)
    entry_count = 2.0 * width * rank
    like = lambda a, dtype=None: jax.ShapeDtypeStruct(a.shape, dtype or a.dtype)
    return pl.pallas_call(
        lambda *refs: last_kernel(*refs, entry_count=entry_count),
        in_specs=[smem] + [vmem] * 8,
        out_specs=[vmem] * 8,
        out_shape=[
            like(query_weight),
            like(key_weight),
            like(query_weight),
            like(key_weight),
            like(query_weight, jnp.bfloat16),
            like(key_weight, jnp.bfloat16),
            like(moment_mean),
            like(moment_square),
        ],
        compiler_params=pltpu.CompilerParams(vmem_limit_bytes=8 << 20),
    )(
        core,
        squares.reshape(far * near, rank),
        tiles,
        moment_mean,
        moment_square,
        query_basis,
        key_basis,
        query_weight,
        key_weight,
    )


def solution(mesh):
    split = Mesh(mesh.devices.reshape(16, 4, 2, mesh.shape["tp"]), ("fs_0", "fs_1", "fs_2", "tp"))
    in_specs = (
        P(FS, None),
        P(FS, "tp"),
        P(FS, "tp"),
        P(FS, "tp"),
        P(FS, "tp"),
        P("tp", None),
        P("tp", None),
        P(None, FS, None),
        P(None, FS, None),
    )
    out_specs = (
        P(FS, "tp"),
        P(FS, "tp"),
        P(FS, "tp"),
        P(FS, "tp"),
        P(FS, "tp"),
        P(FS, "tp"),
        P(None, FS, None),
        P(None, FS, None),
    )
    return jax.shard_map(local, mesh=split, in_specs=in_specs, out_specs=out_specs, check_vma=False)
```

```python
import jax
import jax.numpy as jnp
from jax import lax
from jax.experimental import pallas as pl
from jax.experimental.pallas import tpu as pltpu
from jax.sharding import Mesh
from jax.sharding import PartitionSpec as P

FAR, MIDDLE, NEAR, CHIPS, CORES, HEADS = "z_far", "z_middle", "z_near", "x", "core", "tp"
SIZES = (4, 2, 2, 4, 2)
FS = (FAR, MIDDLE, NEAR, CHIPS, CORES)

BETA_MEAN = 0.75
BETA_SQUARE = 0.8
STEP_RATE = 0.25
EPSILON = 1e-06
BLOCK = 1024
OWN_BLOCK = 512
PIECES = 4

HIGHEST = lax.Precision.HIGHEST
OUTER = (((1,), (1,)), ((), ()))
TOKENS_OUT = (((0,), (0,)), ((), ()))


def dot(a, b, dims, precision=None):
    return lax.dot_general(a, b, dims, precision=precision, preferred_element_type=jnp.float32)


def halves(value):
    high = value.astype(jnp.bfloat16)
    low = (value - high.astype(jnp.float32)).astype(jnp.bfloat16)
    return high, low


def store_block(x, factor, out_ref, first):
    both = dot(x, factor, TOKENS_OUT)
    rank = both.shape[1] // 2
    part = both[:, :rank] + both[:, rank:]
    near, groups, middle, _, tile, _ = out_ref.shape
    for start in range(0, part.shape[0], groups * tile):
        plane = (first + start) // (groups * tile)
        piece = part[start : start + groups * tile]
        far = plane // (near * middle)
        out_ref[plane % near, :, plane // near % middle, far, :, :] = piece.reshape(groups, tile, rank)


def other_kernel(
    core, x_hbm, cq_hbm, ck_hbm, bq_hbm, bk_hbm, out_ref, own_ref, x_ref,
    cq_ref, ck_ref, bq_ref, bk_ref, other_ref, sems, x_sems,
):
    copies = [
        pltpu.make_async_copy(source, target, sems.at[i])
        for i, (source, target) in enumerate(
            ((cq_hbm, cq_ref), (bq_hbm, bq_ref), (ck_hbm, ck_ref), (bk_hbm, bk_ref))
        )
    ]
    tokens, width = x_ref.shape
    rows = [pl.ds(i, tokens // PIECES) for i in range(0, tokens, tokens // PIECES)]
    blocks = [pltpu.make_async_copy(x_hbm.at[r], x_ref.at[r], x_sems.at[i]) for i, r in enumerate(rows)]
    for copy in copies + blocks:
        copy.start()
    for copy in copies:
        copy.wait()
    rank = bq_ref.shape[1]
    query = dot(cq_ref[...], bq_ref[...], (((1,), (0,)), ((), ())))
    key = dot(ck_ref[...], bk_ref[...], (((1,), (0,)), ((), ())))
    is_query = core[0] == 0
    own_high, own_low = halves(jnp.where(is_query, query, key))
    own_ref[:, :rank] = own_high
    own_ref[:, rank:] = own_low
    other_high, other_low = halves(jnp.where(is_query, key, query))
    other_ref[:, :rank] = other_high
    other_ref[:, rank:] = other_low
    for copy in blocks:
        copy.wait()
    for start in range(0, width, BLOCK):
        store_block(x_ref[:, start : start + BLOCK], other_ref[...], out_ref, start)


def own_kernel(own_ref, x_ref, out_ref):
    for start in range(0, x_ref.shape[1], OWN_BLOCK):
        store_block(x_ref[:, start : start + OWN_BLOCK], own_ref[...], out_ref, start)


def last_kernel(
    core, squares_ref, tiles_ref, mean_ref, square_ref, bq_ref, bk_ref, wq_ref, wk_ref,
    qs_ref, ks_ref, qu_ref, ku_ref, qc_ref, kc_ref, mean_out, square_out, *, entry_count,
):
    total = jnp.sum(squares_ref[...].reshape(-1, squares_ref.shape[-1]), axis=0, keepdims=True)
    total = jnp.sum(total, axis=1, keepdims=True)
    scale = lax.rsqrt(total / entry_count + EPSILON)
    groups = tiles_ref.shape[0] // 2
    mine = groups // 2
    rows, rank = mean_ref.shape[1], mean_ref.shape[2]
    for which, basis, weight, step_ref, up_ref, copy_ref in (
        (0, bq_ref, wq_ref, qs_ref, qu_ref, qc_ref),
        (1, bk_ref, wk_ref, ks_ref, ku_ref, kc_ref),
    ):
        tile = tiles_ref[pl.ds(which * groups + core[0] * mine, mine), : rows // mine, :].reshape(rows, rank)
        normalized = tile * scale
        mean = BETA_MEAN * mean_ref[which] + (1.0 - BETA_MEAN) * normalized
        square = BETA_SQUARE * square_ref[which] + (1.0 - BETA_SQUARE) * normalized * normalized
        mean_out[which] = mean
        square_out[which] = square
        direction = mean / jnp.sqrt(square)
        step = dot(direction, basis[...].astype(jnp.float32), OUTER, HIGHEST)
        step_ref[...] = step
        updated = weight[...] - STEP_RATE * step
        up_ref[...] = updated
        copy_ref[...] = updated.astype(jnp.bfloat16)


def whole(shape):
    return pl.BlockSpec(shape, lambda *i: (0,) * len(shape))


def local(
    normed_input,
    query_cotangent,
    key_cotangent,
    query_weight,
    key_weight,
    query_basis,
    key_basis,
    moment_mean,
    moment_square,
):
    far, middle, near, chips, cores, heads = (
        lax.axis_size(a) for a in (FAR, MIDDLE, NEAR, CHIPS, CORES, HEADS)
    )
    core = lax.axis_index(CORES).astype(jnp.int32).reshape(1)
    tokens, width = normed_input.shape
    rank = query_basis.shape[1]
    tile = width // (far * middle * near * chips * heads)
    sums = pltpu.VMEM((near, chips * heads, middle, far, tile, rank), jnp.float32)
    cost = pl.CostEstimate(
        flops=4 * tokens * width * rank, bytes_accessed=2 * tokens * width + 4 * width * rank, transcendentals=0
    )
    params = pltpu.CompilerParams(vmem_limit_bytes=16 << 20)
    factor = pltpu.VMEM((tokens, 2 * rank), jnp.bfloat16)
    sources = (normed_input, query_cotangent, key_cotangent, query_basis, key_basis)
    hbm = pl.BlockSpec(memory_space=pltpu.HBM)
    vmem = pl.BlockSpec(memory_space=pltpu.VMEM)
    smem = pl.BlockSpec(memory_space=pltpu.SMEM)
    other, own_factor, held = pl.pallas_call(
        other_kernel,
        in_specs=[smem] + [hbm] * len(sources),
        out_specs=[vmem] * 3,
        out_shape=[sums, factor, pltpu.VMEM(normed_input.shape, normed_input.dtype)],
        scratch_shapes=[pltpu.VMEM(a.shape, a.dtype) for a in sources[1:3] + sources[3:]]
        + [factor, pltpu.SemaphoreType.DMA((4,)), pltpu.SemaphoreType.DMA((PIECES,))],
        cost_estimate=cost,
        compiler_params=params,
    )(core, *(pltpu.with_memory_space_constraint(a, pltpu.HBM) for a in sources))
    received = lax.ppermute(other, CORES, [(0, 1), (1, 0)])
    own = pl.pallas_call(
        own_kernel,
        in_specs=[vmem] * 2,
        out_specs=vmem,
        out_shape=sums,
        cost_estimate=cost,
        compiler_params=params,
    )(own_factor, held)
    position, received = lax.optimization_barrier((lax.axis_index(FAR), received))
    chip = (own + received).reshape(near * chips * heads, middle, far, tile, rank)
    plane = jnp.sum(lax.all_to_all(chip, (NEAR, CHIPS, HEADS), 0, 0, tiled=True), axis=0)
    sent = jnp.broadcast_to(plane[None], (far, *plane.shape)).reshape(far * middle, far, tile, rank)
    rows = jnp.sum(lax.all_to_all(sent, (FAR, MIDDLE), 0, 0, tiled=True), axis=0)
    mine = lax.dynamic_slice(rows, (position, 0, 0), (1, tile, rank), allow_negative_indices=False)[0]
    sent = jnp.concatenate([mine, jnp.sum(rows * rows, axis=0)], axis=0)
    sent = jnp.broadcast_to(sent[None], (cores * heads, 2 * tile, rank))
    tiles = lax.all_to_all(sent, (CORES, HEADS), 0, 0, tiled=True)
    squares = jnp.sum(tiles[:, tile:], axis=(0, 1))
    squares = jnp.broadcast_to(squares.reshape(1, 1, rank), (middle * near * chips, 1, rank))
    squares = lax.all_to_all(squares, (MIDDLE, NEAR, CHIPS), 0, 0, tiled=True)
    entry_count = 2.0 * width * rank
    like = lambda a, dtype=None: jax.ShapeDtypeStruct(a.shape, dtype or a.dtype)
    return pl.pallas_call(
        lambda *refs: last_kernel(*refs, entry_count=entry_count),
        in_specs=[smem] + [vmem] * 8,
        out_specs=[vmem] * 8,
        out_shape=[
            like(query_weight),
            like(key_weight),
            like(query_weight),
            like(key_weight),
            like(query_weight, jnp.bfloat16),
            like(key_weight, jnp.bfloat16),
            like(moment_mean),
            like(moment_square),
        ],
        compiler_params=pltpu.CompilerParams(vmem_limit_bytes=8 << 20),
    )(
        core,
        squares.reshape(middle * near * chips, rank),
        tiles,
        moment_mean,
        moment_square,
        query_basis,
        key_basis,
        query_weight,
        key_weight,
    )


def solution(mesh):
    split = Mesh(mesh.devices.reshape(*SIZES, mesh.shape["tp"]), (*FS, HEADS))
    in_specs = (
        P(FS, None),
        P(FS, "tp"),
        P(FS, "tp"),
        P(FS, "tp"),
        P(FS, "tp"),
        P("tp", None),
        P("tp", None),
        P(None, FS, None),
        P(None, FS, None),
    )
    out_specs = (
        P(FS, "tp"),
        P(FS, "tp"),
        P(FS, "tp"),
        P(FS, "tp"),
        P(FS, "tp"),
        P(FS, "tp"),
        P(None, FS, None),
        P(None, FS, None),
    )
    return jax.shard_map(local, mesh=split, in_specs=in_specs, out_specs=out_specs, check_vma=False)
```

```python
import jax
import jax.numpy as jnp
from jax import lax
from jax.experimental import pallas as pl
from jax.experimental.pallas import tpu as pltpu
from jax.sharding import Mesh
from jax.sharding import PartitionSpec as P

FAR, MIDDLE, NEAR, CHIPS, CORES, HEADS = "z_far", "z_middle", "z_near", "x", "core", "tp"
SIZES = (4, 2, 2, 4, 2)
FS = (FAR, MIDDLE, NEAR, CHIPS, CORES)

BETA_MEAN = 0.75
BETA_SQUARE = 0.8
STEP_RATE = 0.25
EPSILON = 1e-06
BLOCK = 1024
OWN_BLOCK = 512
PIECES = 4

HIGHEST = lax.Precision.HIGHEST
OUTER = (((1,), (1,)), ((), ()))
TOKENS_OUT = (((0,), (0,)), ((), ()))


def dot(a, b, dims, precision=None):
    return lax.dot_general(a, b, dims, precision=precision, preferred_element_type=jnp.float32)


def halves(value):
    high = value.astype(jnp.bfloat16)
    low = (value - high.astype(jnp.float32)).astype(jnp.bfloat16)
    return high, low


def store_block(x, factor, out_ref, first):
    both = dot(x, factor, TOKENS_OUT)
    rank = both.shape[1] // 2
    part = both[:, :rank] + both[:, rank:]
    near, groups, middle, _, tile, _ = out_ref.shape
    for start in range(0, part.shape[0], groups * tile):
        plane = (first + start) // (groups * tile)
        piece = part[start : start + groups * tile]
        far = plane // (near * middle)
        out_ref[plane % near, :, plane // near % middle, far, :, :] = piece.reshape(groups, tile, rank)


def other_kernel(
    core, x_hbm, cq_hbm, ck_hbm, bq_hbm, bk_hbm, out_ref, own_ref, x_ref,
    cq_ref, ck_ref, bq_ref, bk_ref, other_ref, sems, x_sems,
):
    copies = [
        pltpu.make_async_copy(source, target, sems.at[i])
        for i, (source, target) in enumerate(
            ((cq_hbm, cq_ref), (bq_hbm, bq_ref), (ck_hbm, ck_ref), (bk_hbm, bk_ref))
        )
    ]
    tokens, width = x_ref.shape
    rows = [pl.ds(i, tokens // PIECES) for i in range(0, tokens, tokens // PIECES)]
    blocks = [pltpu.make_async_copy(x_hbm.at[r], x_ref.at[r], x_sems.at[i]) for i, r in enumerate(rows)]
    for copy in copies + blocks:
        copy.start()
    for copy in copies:
        copy.wait()
    rank = bq_ref.shape[1]
    query = dot(cq_ref[...], bq_ref[...], (((1,), (0,)), ((), ())))
    key = dot(ck_ref[...], bk_ref[...], (((1,), (0,)), ((), ())))
    is_query = core[0] == 0
    own_high, own_low = halves(jnp.where(is_query, query, key))
    own_ref[:, :rank] = own_high
    own_ref[:, rank:] = own_low
    other_high, other_low = halves(jnp.where(is_query, key, query))
    other_ref[:, :rank] = other_high
    other_ref[:, rank:] = other_low
    for copy in blocks:
        copy.wait()
    for start in range(0, width, BLOCK):
        store_block(x_ref[:, start : start + BLOCK], other_ref[...], out_ref, start)


def own_kernel(own_ref, x_ref, out_ref):
    for start in range(0, x_ref.shape[1], OWN_BLOCK):
        store_block(x_ref[:, start : start + OWN_BLOCK], own_ref[...], out_ref, start)


def last_kernel(
    core, squares_ref, tiles_ref, mean_ref, square_ref, bq_ref, bk_ref, wq_ref, wk_ref,
    qs_ref, ks_ref, qu_ref, ku_ref, qc_ref, kc_ref, mean_out, square_out, *, entry_count,
):
    total = jnp.sum(squares_ref[...].reshape(-1, squares_ref.shape[-1]), axis=0, keepdims=True)
    total = jnp.sum(total, axis=1, keepdims=True)
    scale = lax.rsqrt(total / entry_count + EPSILON)
    groups = tiles_ref.shape[0] // 2
    mine = groups // 2
    rows, rank = mean_ref.shape[1], mean_ref.shape[2]
    for which, basis, weight, step_ref, up_ref, copy_ref in (
        (0, bq_ref, wq_ref, qs_ref, qu_ref, qc_ref),
        (1, bk_ref, wk_ref, ks_ref, ku_ref, kc_ref),
    ):
        tile = tiles_ref[pl.ds(which * groups + core[0] * mine, mine), : rows // mine, :].reshape(rows, rank)
        normalized = tile * scale
        mean = BETA_MEAN * mean_ref[which] + (1.0 - BETA_MEAN) * normalized
        square = BETA_SQUARE * square_ref[which] + (1.0 - BETA_SQUARE) * normalized * normalized
        mean_out[which] = mean
        square_out[which] = square
        direction = mean / jnp.sqrt(square)
        step = dot(direction, basis[...].astype(jnp.float32), OUTER, HIGHEST)
        step_ref[...] = step
        updated = weight[...] - STEP_RATE * step
        up_ref[...] = updated
        copy_ref[...] = updated.astype(jnp.bfloat16)


def whole(shape):
    return pl.BlockSpec(shape, lambda *i: (0,) * len(shape))


def local(
    normed_input,
    query_cotangent,
    key_cotangent,
    query_weight,
    key_weight,
    query_basis,
    key_basis,
    moment_mean,
    moment_square,
):
    far, middle, near, chips, cores, heads = (
        lax.axis_size(a) for a in (FAR, MIDDLE, NEAR, CHIPS, CORES, HEADS)
    )
    core = lax.axis_index(CORES).astype(jnp.int32).reshape(1)
    position, core = lax.optimization_barrier((lax.axis_index(FAR), core))
    tokens, width = normed_input.shape
    rank = query_basis.shape[1]
    tile = width // (far * middle * near * chips * heads)
    sums = pltpu.VMEM((near, chips * heads, middle, far, tile, rank), jnp.float32)
    cost = pl.CostEstimate(
        flops=4 * tokens * width * rank, bytes_accessed=2 * tokens * width + 4 * width * rank, transcendentals=0
    )
    params = pltpu.CompilerParams(vmem_limit_bytes=16 << 20)
    factor = pltpu.VMEM((tokens, 2 * rank), jnp.bfloat16)
    sources = (normed_input, query_cotangent, key_cotangent, query_basis, key_basis)
    hbm = pl.BlockSpec(memory_space=pltpu.HBM)
    vmem = pl.BlockSpec(memory_space=pltpu.VMEM)
    smem = pl.BlockSpec(memory_space=pltpu.SMEM)
    other, own_factor, held = pl.pallas_call(
        other_kernel,
        in_specs=[smem] + [hbm] * len(sources),
        out_specs=[vmem] * 3,
        out_shape=[sums, factor, pltpu.VMEM(normed_input.shape, normed_input.dtype)],
        scratch_shapes=[pltpu.VMEM(a.shape, a.dtype) for a in sources[1:3] + sources[3:]]
        + [factor, pltpu.SemaphoreType.DMA((4,)), pltpu.SemaphoreType.DMA((PIECES,))],
        cost_estimate=cost,
        compiler_params=params,
    )(core, *(pltpu.with_memory_space_constraint(a, pltpu.HBM) for a in sources))
    received = lax.ppermute(other, CORES, [(0, 1), (1, 0)])
    own = pl.pallas_call(
        own_kernel,
        in_specs=[vmem] * 2,
        out_specs=vmem,
        out_shape=sums,
        cost_estimate=cost,
        compiler_params=params,
    )(own_factor, held)
    chip = (own + received).reshape(near * chips * heads, middle, far, tile, rank)
    plane = jnp.sum(lax.all_to_all(chip, (NEAR, CHIPS, HEADS), 0, 0, tiled=True), axis=0)
    sent = jnp.broadcast_to(plane[None], (far, *plane.shape)).reshape(far * middle, far, tile, rank)
    rows = jnp.sum(lax.all_to_all(sent, (FAR, MIDDLE), 0, 0, tiled=True), axis=0)
    mine = lax.dynamic_slice(rows, (position, 0, 0), (1, tile, rank), allow_negative_indices=False)[0]
    sent = jnp.concatenate([mine, jnp.sum(rows * rows, axis=0)], axis=0)
    sent = jnp.broadcast_to(sent[None], (cores * heads, 2 * tile, rank))
    tiles = lax.all_to_all(sent, (CORES, HEADS), 0, 0, tiled=True)
    squares = jnp.sum(tiles[:, tile:], axis=(0, 1))
    squares = jnp.broadcast_to(squares.reshape(1, 1, rank), (middle * near * chips, 1, rank))
    squares = lax.all_to_all(squares, (MIDDLE, NEAR, CHIPS), 0, 0, tiled=True)
    entry_count = 2.0 * width * rank
    like = lambda a, dtype=None: jax.ShapeDtypeStruct(a.shape, dtype or a.dtype)
    return pl.pallas_call(
        lambda *refs: last_kernel(*refs, entry_count=entry_count),
        in_specs=[smem] + [vmem] * 8,
        out_specs=[vmem] * 8,
        out_shape=[
            like(query_weight),
            like(key_weight),
            like(query_weight),
            like(key_weight),
            like(query_weight, jnp.bfloat16),
            like(key_weight, jnp.bfloat16),
            like(moment_mean),
            like(moment_square),
        ],
        compiler_params=pltpu.CompilerParams(vmem_limit_bytes=8 << 20),
    )(
        core,
        squares.reshape(middle * near * chips, rank),
        tiles,
        moment_mean,
        moment_square,
        query_basis,
        key_basis,
        query_weight,
        key_weight,
    )


def solution(mesh):
    split = Mesh(mesh.devices.reshape(*SIZES, mesh.shape["tp"]), (*FS, HEADS))
    in_specs = (
        P(FS, None),
        P(FS, "tp"),
        P(FS, "tp"),
        P(FS, "tp"),
        P(FS, "tp"),
        P("tp", None),
        P("tp", None),
        P(None, FS, None),
        P(None, FS, None),
    )
    out_specs = (
        P(FS, "tp"),
        P(FS, "tp"),
        P(FS, "tp"),
        P(FS, "tp"),
        P(FS, "tp"),
        P(FS, "tp"),
        P(None, FS, None),
        P(None, FS, None),
    )
    return jax.shard_map(local, mesh=split, in_specs=in_specs, out_specs=out_specs, check_vma=False)
```

```python
import jax
import jax.numpy as jnp
from jax import lax
from jax.experimental import pallas as pl
from jax.experimental.pallas import tpu as pltpu
from jax.sharding import Mesh
from jax.sharding import PartitionSpec as P

FAR, MIDDLE, NEAR, CHIPS, CORES, HEADS = "z_far", "z_middle", "z_near", "x", "core", "tp"
SIZES = (4, 2, 2, 4, 2)
FS = (FAR, MIDDLE, NEAR, CHIPS, CORES)

BETA_MEAN = 0.75
BETA_SQUARE = 0.8
STEP_RATE = 0.25
EPSILON = 1e-06
BLOCK = 1024
OWN_BLOCK = 512
PIECES = 4

HIGHEST = lax.Precision.HIGHEST
OUTER = (((1,), (1,)), ((), ()))
TOKENS_OUT = (((0,), (0,)), ((), ()))


def dot(a, b, dims, precision=None):
    return lax.dot_general(a, b, dims, precision=precision, preferred_element_type=jnp.float32)


def halves(value):
    high = value.astype(jnp.bfloat16)
    low = (value - high.astype(jnp.float32)).astype(jnp.bfloat16)
    return high, low


def store_block(x, factor, out_ref, first):
    both = dot(x, factor, TOKENS_OUT)
    rank = both.shape[1] // 2
    part = both[:, :rank] + both[:, rank:]
    near, groups, middle, _, tile, _ = out_ref.shape
    for start in range(0, part.shape[0], groups * tile):
        plane = (first + start) // (groups * tile)
        piece = part[start : start + groups * tile]
        far = plane // (near * middle)
        out_ref[plane % near, :, plane // near % middle, far, :, :] = piece.reshape(groups, tile, rank)


def store_factor(is_query, cq_ref, ck_ref, bq_ref, bk_ref, factor_ref):
    rank = bq_ref.shape[1]

    def store(cotangent, basis):
        high, low = halves(dot(cotangent[...], basis[...], (((1,), (0,)), ((), ()))))
        factor_ref[:, :rank] = high
        factor_ref[:, rank:] = low

    pl.when(is_query)(lambda: store(cq_ref, bq_ref))
    pl.when(jnp.logical_not(is_query))(lambda: store(ck_ref, bk_ref))


def other_kernel(
    core, x_hbm, cq_hbm, ck_hbm, bq_hbm, bk_hbm, out_ref, x_ref,
    cq_ref, ck_ref, bq_ref, bk_ref, other_ref, sems, x_sems,
):
    copies = [
        pltpu.make_async_copy(source, target, sems.at[i])
        for i, (source, target) in enumerate(
            ((cq_hbm, cq_ref), (bq_hbm, bq_ref), (ck_hbm, ck_ref), (bk_hbm, bk_ref))
        )
    ]
    tokens, width = x_ref.shape
    rows = [pl.ds(i, tokens // PIECES) for i in range(0, tokens, tokens // PIECES)]
    blocks = [pltpu.make_async_copy(x_hbm.at[r], x_ref.at[r], x_sems.at[i]) for i, r in enumerate(rows)]
    for copy in copies + blocks:
        copy.start()
    for copy in copies:
        copy.wait()
    store_factor(core[0] != 0, cq_ref, ck_ref, bq_ref, bk_ref, other_ref)
    for copy in blocks:
        copy.wait()
    for start in range(0, width, BLOCK):
        store_block(x_ref[:, start : start + BLOCK], other_ref[...], out_ref, start)


def own_kernel(core, x_ref, cq_ref, ck_ref, bq_ref, bk_ref, out_ref, own_ref):
    store_factor(core[0] == 0, cq_ref, ck_ref, bq_ref, bk_ref, own_ref)
    for start in range(0, x_ref.shape[1], OWN_BLOCK):
        store_block(x_ref[:, start : start + OWN_BLOCK], own_ref[...], out_ref, start)


def last_kernel(
    core, squares_ref, tiles_ref, mean_ref, square_ref, bq_ref, bk_ref, wq_ref, wk_ref,
    qs_ref, ks_ref, qu_ref, ku_ref, qc_ref, kc_ref, mean_out, square_out, *, entry_count,
):
    total = jnp.sum(squares_ref[...].reshape(-1, squares_ref.shape[-1]), axis=0, keepdims=True)
    total = jnp.sum(total, axis=1, keepdims=True)
    scale = lax.rsqrt(total / entry_count + EPSILON)
    groups = tiles_ref.shape[0] // 2
    mine = groups // 2
    rows, rank = mean_ref.shape[1], mean_ref.shape[2]
    for which, basis, weight, step_ref, up_ref, copy_ref in (
        (0, bq_ref, wq_ref, qs_ref, qu_ref, qc_ref),
        (1, bk_ref, wk_ref, ks_ref, ku_ref, kc_ref),
    ):
        tile = tiles_ref[pl.ds(which * groups + core[0] * mine, mine), : rows // mine, :].reshape(rows, rank)
        normalized = tile * scale
        mean = BETA_MEAN * mean_ref[which] + (1.0 - BETA_MEAN) * normalized
        square = BETA_SQUARE * square_ref[which] + (1.0 - BETA_SQUARE) * normalized * normalized
        mean_out[which] = mean
        square_out[which] = square
        direction = mean / jnp.sqrt(square)
        step = dot(direction, basis[...].astype(jnp.float32), OUTER, HIGHEST)
        step_ref[...] = step
        updated = weight[...] - STEP_RATE * step
        up_ref[...] = updated
        copy_ref[...] = updated.astype(jnp.bfloat16)


def whole(shape):
    return pl.BlockSpec(shape, lambda *i: (0,) * len(shape))


def local(
    normed_input,
    query_cotangent,
    key_cotangent,
    query_weight,
    key_weight,
    query_basis,
    key_basis,
    moment_mean,
    moment_square,
):
    far, middle, near, chips, cores, heads = (
        lax.axis_size(a) for a in (FAR, MIDDLE, NEAR, CHIPS, CORES, HEADS)
    )
    core = lax.axis_index(CORES).astype(jnp.int32).reshape(1)
    position, core = lax.optimization_barrier((lax.axis_index(FAR), core))
    tokens, width = normed_input.shape
    rank = query_basis.shape[1]
    tile = width // (far * middle * near * chips * heads)
    sums = pltpu.VMEM((near, chips * heads, middle, far, tile, rank), jnp.float32)
    cost = pl.CostEstimate(
        flops=4 * tokens * width * rank, bytes_accessed=2 * tokens * width + 4 * width * rank, transcendentals=0
    )
    params = pltpu.CompilerParams(vmem_limit_bytes=16 << 20)
    factor = pltpu.VMEM((tokens, 2 * rank), jnp.bfloat16)
    sources = (normed_input, query_cotangent, key_cotangent, query_basis, key_basis)
    hbm = pl.BlockSpec(memory_space=pltpu.HBM)
    vmem = pl.BlockSpec(memory_space=pltpu.VMEM)
    smem = pl.BlockSpec(memory_space=pltpu.SMEM)
    other, *held = pl.pallas_call(
        other_kernel,
        in_specs=[smem] + [hbm] * len(sources),
        out_specs=[vmem] * (1 + len(sources)),
        out_shape=[sums] + [pltpu.VMEM(a.shape, a.dtype) for a in sources],
        scratch_shapes=[factor, pltpu.SemaphoreType.DMA((4,)), pltpu.SemaphoreType.DMA((PIECES,))],
        cost_estimate=cost,
        compiler_params=params,
    )(core, *(pltpu.with_memory_space_constraint(a, pltpu.HBM) for a in sources))
    received = lax.ppermute(other, CORES, [(0, 1), (1, 0)])
    own = pl.pallas_call(
        own_kernel,
        in_specs=[smem] + [vmem] * len(sources),
        out_specs=vmem,
        out_shape=sums,
        scratch_shapes=[factor],
        cost_estimate=cost,
        compiler_params=params,
    )(core, *held)
    chip = (own + received).reshape(near * chips * heads, middle, far, tile, rank)
    plane = jnp.sum(lax.all_to_all(chip, (NEAR, CHIPS, HEADS), 0, 0, tiled=True), axis=0)
    sent = jnp.broadcast_to(plane[None], (far, *plane.shape)).reshape(far * middle, far, tile, rank)
    rows = jnp.sum(lax.all_to_all(sent, (FAR, MIDDLE), 0, 0, tiled=True), axis=0)
    mine = lax.dynamic_slice(rows, (position, 0, 0), (1, tile, rank), allow_negative_indices=False)[0]
    sent = jnp.concatenate([mine, jnp.sum(rows * rows, axis=0)], axis=0)
    sent = jnp.broadcast_to(sent[None], (cores * heads, 2 * tile, rank))
    tiles = lax.all_to_all(sent, (CORES, HEADS), 0, 0, tiled=True)
    squares = jnp.sum(tiles[:, tile:], axis=(0, 1))
    squares = jnp.broadcast_to(squares.reshape(1, 1, rank), (middle * near * chips, 1, rank))
    squares = lax.all_to_all(squares, (MIDDLE, NEAR, CHIPS), 0, 0, tiled=True)
    entry_count = 2.0 * width * rank
    like = lambda a, dtype=None: jax.ShapeDtypeStruct(a.shape, dtype or a.dtype)
    return pl.pallas_call(
        lambda *refs: last_kernel(*refs, entry_count=entry_count),
        in_specs=[smem] + [vmem] * 8,
        out_specs=[vmem] * 8,
        out_shape=[
            like(query_weight),
            like(key_weight),
            like(query_weight),
            like(key_weight),
            like(query_weight, jnp.bfloat16),
            like(key_weight, jnp.bfloat16),
            like(moment_mean),
            like(moment_square),
        ],
        compiler_params=pltpu.CompilerParams(vmem_limit_bytes=8 << 20),
    )(
        core,
        squares.reshape(middle * near * chips, rank),
        tiles,
        moment_mean,
        moment_square,
        query_basis,
        key_basis,
        query_weight,
        key_weight,
    )


def solution(mesh):
    split = Mesh(mesh.devices.reshape(*SIZES, mesh.shape["tp"]), (*FS, HEADS))
    in_specs = (
        P(FS, None),
        P(FS, "tp"),
        P(FS, "tp"),
        P(FS, "tp"),
        P(FS, "tp"),
        P("tp", None),
        P("tp", None),
        P(None, FS, None),
        P(None, FS, None),
    )
    out_specs = (
        P(FS, "tp"),
        P(FS, "tp"),
        P(FS, "tp"),
        P(FS, "tp"),
        P(FS, "tp"),
        P(FS, "tp"),
        P(None, FS, None),
        P(None, FS, None),
    )
    return jax.shard_map(local, mesh=split, in_specs=in_specs, out_specs=out_specs, check_vma=False)
```
